32 devices in a mesh: fs: 16 (over z, y, x), tp: 2 (over core).
Axes of the slice: x: 2, y: 2, z: 4, core: 2. Of those that a mesh axis runs over, the one named last changes fastest.
Arguments:
- cotangent: bfloat16 [2048, 2048], P('fs')
- values_first: bfloat16 [2048, 2048], P('fs', 'tp'), may hold values from -6 to 6
- values_second: bfloat16 [2048, 2048], P('fs', 'tp'), may hold values from -6 to 6
- head_lambda: float32 [16], P('tp'), may hold values from 0.3 to 0.8
- out_gain: float32 [128], replicated, may hold values from 0.3 to 3
- weight: float32 [2048, 2048], P('fs', 'tp'), may hold values from -0.125 to 0.125
- left_stat: float32 [2048, 2048], P('fs', 'tp'), as said below
- right_stat: float32 [16, 128, 128], P('tp')
- left_root: bfloat16 [2048, 2048], P('fs'), as said below
- right_root: bfloat16 [16, 128, 128], P('tp')
Outputs:
- update_step: float32 [2048, 2048], P('fs', 'tp')
- new_weight: float32 [2048, 2048], P('fs', 'tp')
- new_copy: bfloat16 [2048, 2048], P(None, 'tp')
- new_left_stat: float32 [2048, 2048], P('fs', 'tp')
- new_right_stat: float32 [16, 128, 128], P('tp')
The draws below stay inside these ranges and needn't reach their ends.
Inputs may be any that keep to these rules, and one draw needn't show every extreme that they name: `left_root`: each of the 2048 x 2048 matrix and the 16 matrices of size 128 equals its transpose; the same holds for right_root. `left_stat`: the matrix and each of the 16 matrices equals its transpose; the same holds for right_stat.
All inputs are finite; a program needn't handle non-finite values.
Results may differ from the reference program's by a relative error of at most 0.007.
Values may be sent and summed in bfloat16 or wider, within the bound.
A program may use at most 64 MiB of HBM per device.

```python
import math
import jax
import jax.numpy as jnp
from jax import lax

D = 2048
HEADS = 16
VH = 128
V = 2048
TOKENS = 2048


def symmetric_blocks(key, order, spread, count):
    first_key, second_key = jax.random.split(key)
    random_part = jax.random.normal(first_key, (count, order, order), jnp.float32)
    mirrored = (random_part + jnp.swapaxes(random_part, 1, 2)) * (spread / math.sqrt(2.0 * order))
    diagonal = jnp.exp(jax.random.uniform(second_key, (count, order), jnp.float32, math.log(0.5), math.log(2.0)))
    return mirrored + diagonal[:, :, None] * jnp.eye(order, dtype=jnp.float32)[None]


def draw_left_root(key, part):
    return symmetric_blocks(jax.random.fold_in(key, 11), D, 0.5, 1)[0].astype(jnp.bfloat16)


def draw_right_root(key, part):
    return symmetric_blocks(jax.random.fold_in(key, 12), VH, 0.5, HEADS).astype(jnp.bfloat16)


def draw_left_stat(key, part):
    return symmetric_blocks(jax.random.fold_in(key, 13), D, 0.4, 1)[0]


def draw_right_stat(key, part):
    return symmetric_blocks(jax.random.fold_in(key, 14), VH, 0.4, HEADS)


def draw_cotangent(key, part):
    first_key, second_key = jax.random.split(jax.random.fold_in(key, 15), 2)
    position = jnp.arange(D, dtype=jnp.float32) / D
    rough = jnp.exp(jax.random.uniform(second_key, (D,), jnp.float32, -0.4, 0.4))
    columns = 3.0 ** position * rough
    entries = jax.random.normal(first_key, (TOKENS, D), jnp.float32)
    return (entries * columns[None, :] * (3.2 / math.sqrt(TOKENS))).astype(jnp.bfloat16)


def level_of(rng, dims, pieces, smallest, high):
    level, own = 1.0, jax.random.fold_in(rng, 6)
    for dim, parts in pieces:
        draws = jnp.exp(jax.random.uniform(jax.random.fold_in(own, dim), (parts,), jnp.float32, smallest / len(pieces), high / len(pieces)))
        level = level * jnp.repeat(draws, dims[dim] // parts).reshape([-1 if axis == dim else 1 for axis in range(len(dims))])
    return level


def gaussian(stream_key, extent, width, reach, cuts=(), kind=jnp.bfloat16):
    result = width * jax.random.normal(stream_key, extent, jnp.float32)
    if cuts:
        result = result * level_of(stream_key, extent, cuts, -0.22, 0.18)
    return jnp.clip(result, -reach, reach).astype(kind)


def setup_inputs(seed: int = 0) -> dict:
    arg_keys = jax.random.split(jax.random.key(seed), 11)
    return {
        "cotangent": draw_cotangent(jax.random.fold_in(arg_keys[10], 71), 0),
        "values_first": gaussian(arg_keys[1], (TOKENS, V), 1.0, 6.0, ((0, 16), (1, 2))),
        "values_second": gaussian(arg_keys[2], (TOKENS, V), 1.0, 6.0, ((0, 16), (1, 2))),
        "head_lambda": jnp.clip(0.3 + 0.5 * jax.random.uniform(arg_keys[3], (HEADS,), jnp.float32) ** level_of(arg_keys[3], (HEADS,), ((0, 2),), -0.2, 0.2), 0.3, 0.8),
        "out_gain": jnp.clip(jnp.exp(jax.random.uniform(arg_keys[4], (VH,), jnp.float32, math.log(0.3), math.log(3.0))), 0.3, 3.0),
        "weight": gaussian(arg_keys[5], (D, V), V ** -0.5, 0.125, ((0, 16), (1, 2)), jnp.float32),
        "left_stat": draw_left_stat(jax.random.fold_in(arg_keys[10], 71), 0),
        "right_stat": draw_right_stat(jax.random.fold_in(arg_keys[10], 71), 0),
        "left_root": draw_left_root(jax.random.fold_in(arg_keys[10], 71), 0),
        "right_root": draw_right_root(jax.random.fold_in(arg_keys[10], 71), 0),
    }


epsilon = 1e-06
decay_rate = 0.9
learn_rate = 0.01
output_scale = 0.2

def reference(cotangent, values_first, values_second, head_lambda, out_gain, weight, left_stat, right_stat, left_root, right_root):
    first = values_first.astype(jnp.float32).reshape(-1, HEADS, VH)
    second = values_second.astype(jnp.float32).reshape(-1, HEADS, VH)
    difference = first - head_lambda[None, :, None] * second
    inverse = lax.rsqrt(lax.optimization_barrier(jnp.mean(difference * difference, axis=-1, keepdims=True)) + epsilon)
    head_out = (difference * inverse * out_gain * output_scale).reshape(-1, HEADS * VH).astype(jnp.bfloat16)
    gradient = lax.dot_general(cotangent, head_out, (((0,), (0,)), ((), ())), preferred_element_type=jnp.float32)
    grad_half = gradient.astype(jnp.bfloat16)
    left_product = lax.dot_general(grad_half, grad_half, (((1,), (1,)), ((), ())), preferred_element_type=jnp.float32)
    new_left_stat = decay_rate * left_stat + (1.0 - decay_rate) / (HEADS * VH) * left_product
    heads = grad_half.astype(jnp.float32).reshape(D, HEADS, VH)
    right_product = jnp.einsum('dhi,dhj->hij', heads, heads)
    new_right_stat = decay_rate * right_stat + (1.0 - decay_rate) / D * right_product
    left_part = jnp.dot(left_root, grad_half, preferred_element_type=jnp.float32).astype(jnp.bfloat16)
    precond = jnp.einsum('dhi,hij->dhj', left_part.astype(jnp.float32).reshape(D, HEADS, VH), right_root.astype(jnp.float32)).reshape(D, HEADS * VH)
    grad_square = jnp.sum(gradient * gradient)
    update_square = jnp.sum(precond * precond)
    factor = jnp.sqrt((grad_square + epsilon) / (update_square + epsilon))
    update_step = factor * precond
    new_weight = weight - learn_rate * update_step
    return (update_step, new_weight, new_weight.astype(jnp.bfloat16), new_left_stat, new_right_stat)
```

```python
import functools

import jax
import jax.numpy as jnp
from jax import lax
from jax.experimental import pallas as pl
from jax.experimental.pallas import tpu as pltpu
from jax.sharding import PartitionSpec as P

MESH = pl.DeviceIdType.MESH
INNER = 4

epsilon = 1e-06
decay_rate = 0.9
learn_rate = 0.01
output_scale = 0.2


def normalized(values_first, values_second, head_lambda, out_gain):
    token_count = values_first.shape[0]
    head_count = head_lambda.shape[0]
    head_size = out_gain.shape[0]
    first = values_first.astype(jnp.float32).reshape(token_count, head_count, head_size)
    second = values_second.astype(jnp.float32).reshape(token_count, head_count, head_size)
    difference = first - head_lambda[None, :, None] * second
    inverse = lax.rsqrt(jnp.mean(difference * difference, axis=-1, keepdims=True) + epsilon)
    scaled = difference * inverse * out_gain * output_scale
    return scaled.reshape(token_count, head_count * head_size).astype(jnp.bfloat16)


def by_head(matrix, head_count):
    return matrix.reshape(matrix.shape[0], head_count, matrix.shape[1] // head_count)


def head_products(matrix, head_count):
    heads = by_head(matrix, head_count)
    return jnp.einsum("rhi,rhj->hij", heads, heads, preferred_element_type=jnp.float32)


def shards(
    cotangent,
    values_first,
    values_second,
    head_lambda,
    out_gain,
    weight,
    left_stat,
    right_stat,
    left_root,
    right_root,
):
    head_count = head_lambda.shape[0]
    own_rows = weight.shape[0]
    own_cols = weight.shape[1]
    width = left_root.shape[1]
    total_cols = own_cols * lax.axis_size("tp")
    head_out = normalized(values_first, values_second, head_lambda, out_gain)
    contract_rows = (((0,), (0,)), ((), ()))
    contract_cols = (((1,), (1,)), ((), ()))
    gradient = lax.psum_scatter(
        lax.dot_general(cotangent, head_out, contract_rows, preferred_element_type=jnp.float32),
        "fs",
        scatter_dimension=0,
        tiled=True,
    )
    grad_half = gradient.astype(jnp.bfloat16)
    portion = lax.all_gather(grad_half, "fs", axis=0, tiled=True)
    left_acc = jnp.dot(left_root, portion, preferred_element_type=jnp.float32)
    products = lax.dot_general(
        grad_half, portion, contract_cols, preferred_element_type=jnp.float32
    )
    stat_cols = products
    right_acc = head_products(portion, head_count)
    left_acc, stat_cols, right_acc = (left_acc, stat_cols, right_acc)
    left_summed = lax.psum_scatter(
        stat_cols.astype(jnp.bfloat16), "tp", scatter_dimension=1, tiled=True
    ).astype(jnp.float32)
    new_left_stat = decay_rate * left_stat + (1.0 - decay_rate) / total_cols * left_summed
    new_right_stat = decay_rate * right_stat + (1.0 - decay_rate) / width * right_acc
    left_half = left_acc.astype(jnp.bfloat16)
    precond = jnp.einsum(
        "rhi,hij->rhj",
        by_head(left_half, head_count),
        right_root,
        preferred_element_type=jnp.float32,
    )
    precond = precond.reshape(own_rows, own_cols)
    grad_square, update_square = lax.psum(
        (jnp.sum(gradient * gradient), jnp.sum(precond * precond)), ("fs", "tp")
    )
    factor = jnp.sqrt((grad_square + epsilon) / (update_square + epsilon))
    update_step = factor * precond
    new_weight = weight - learn_rate * update_step
    new_copy = lax.all_gather(new_weight.astype(jnp.bfloat16), "fs", axis=0, tiled=True)
    return (update_step, new_weight, new_copy, new_left_stat, new_right_stat)


def dot(a, b, dims):
    return lax.dot_general(a, b, (dims, ((), ())), preferred_element_type=jnp.float32)


def fused_kernel(
    outer,
    inner,
    lam_ref,
    cot_ref,
    first_ref,
    second_ref,
    gain_ref,
    root_ref,
    right_root_hbm,
    weight_hbm,
    left_stat_hbm,
    right_stat_hbm,
    step_ref,
    new_weight_ref,
    copy_ref,
    new_left_ref,
    new_right_ref,
    cot_all,
    root_all,
    head_out,
    head_in,
    part_out,
    part_in,
    grad_t,
    grad_rows,
    pre_out,
    pre_in,
    prod_all,
    square_out,
    square_in,
    stat_own,
    pair_out,
    pair_in,
    stat_out,
    stat_in,
    rr_ref,
    w_ref,
    ls_ref,
    rs_ref,
    send_sem,
    recv_sem,
    local_sem,
):
    me = lax.axis_index("fs")
    core = lax.axis_index("tp")
    oi = me // inner
    ij = lax.rem(me, inner)
    rows = cot_ref.shape[0]
    width = cot_ref.shape[1]
    own_rows = root_ref.shape[0]
    size = gain_ref.shape[1]
    cols = head_in.shape[1]
    heads_each = cols // size
    chunk = width // outer
    half = width // 2
    mine = pl.ds(pl.multiple_of(core * half, half), half)

    def inner_peer(d):
        return lax.rem(ij + d, inner)

    def outer_peer(d):
        return lax.rem(oi + d, outer)

    def inner_id(d):
        return (oi * inner + inner_peer(d), core)

    def outer_id(d):
        return (outer_peer(d) * inner + ij, core)

    sibling = (me, 1 - core)
    started = []

    def send(src, dst, device):
        index = len(started)
        copy = pltpu.make_async_remote_copy(
            src_ref=src,
            dst_ref=dst,
            send_sem=send_sem.at[index],
            recv_sem=recv_sem.at[index],
            device_id=device,
            device_id_type=MESH,
        )
        copy.start()
        started.append(copy)
        return copy

    inner_steps = range(1, inner)
    outer_steps = range(1, outer)

    locals_ = [
        pltpu.make_async_copy(cot_ref, cot_all.at[ij], local_sem.at[0]),
        pltpu.make_async_copy(root_ref, root_all.at[ij], local_sem.at[1]),
        pltpu.make_async_copy(right_root_hbm, rr_ref, local_sem.at[2]),
        pltpu.make_async_copy(weight_hbm, w_ref, local_sem.at[3]),
        pltpu.make_async_copy(left_stat_hbm, ls_ref, local_sem.at[4]),
        pltpu.make_async_copy(right_stat_hbm, rs_ref, local_sem.at[5]),
    ]
    for copy in locals_:
        copy.start()

    barrier = pltpu.get_barrier_semaphore()
    peers = [inner_id(d) for d in inner_steps] + [outer_id(d) for d in outer_steps] + [sibling]
    for peer in peers:
        pl.semaphore_signal(barrier, inc=1, device_id=peer, device_id_type=MESH)
    pl.semaphore_wait(barrier, len(peers))

    cot_copies = [
        send(cot_ref.at[:, mine], cot_all.at[ij, :, mine], inner_id(d)) for d in inner_steps
    ]

    gain = gain_ref[...] * output_scale
    for h in range(inner * heads_each):
        span = slice(h * size, (h + 1) * size)
        first = first_ref[:, span].astype(jnp.float32)
        second = second_ref[:, span].astype(jnp.float32)
        difference = first - lam_ref[h] * second
        inverse = lax.rsqrt(jnp.mean(difference * difference, axis=-1, keepdims=True) + epsilon)
        scaled = difference * inverse * gain
        k = h % heads_each
        head_out[h // heads_each, k * size : (k + 1) * size, :] = scaled.T.astype(jnp.bfloat16)
    head_copies = [
        send(head_out.at[inner_peer(d)], head_in.at[ij], inner_id(d)) for d in inner_steps
    ]
    head_in[ij] = head_out[ij]

    def forward(copies, buffer):
        result = []
        for d, copy in zip(inner_steps, copies):
            copy.wait_recv()
            place = buffer.at[lax.rem(ij + inner - d, inner), :, mine]
            result.append(send(place, place, sibling))
        return result

    cot_pair = forward(cot_copies, cot_all)
    for copy in head_copies:
        copy.wait_recv()
    root_copies = [
        send(root_ref.at[:, mine], root_all.at[ij, :, mine], inner_id(d)) for d in inner_steps
    ]
    for copy in cot_pair:
        copy.wait_recv()
    locals_[0].wait()

    lhs = jnp.concatenate([head_in[j] for j in range(inner)], axis=1)

    def part(owner):
        span = pl.ds(pl.multiple_of(owner * chunk, chunk), chunk)
        rhs = cot_all[:, :, span].reshape(inner * rows, chunk)
        return dot(lhs, rhs, ((1,), (0,)))

    part_copies = []
    for d in outer_steps:
        owner = outer_peer(d)
        part_out[d - 1] = part(owner).astype(jnp.bfloat16)
        part_copies.append(send(part_out.at[d - 1], part_in.at[d - 1], outer_id(d)))
    gradient = part(oi)
    for d in outer_steps:
        part_copies[d - 1].wait_recv()
        gradient = gradient + part_in[d - 1].astype(jnp.float32)
    grad_t[oi] = gradient.astype(jnp.bfloat16)
    grad_copies = [send(grad_t.at[oi], grad_t.at[oi], outer_id(d)) for d in outer_steps]
    square_out[0, 0] = jnp.full((8, 128), jnp.sum(gradient * gradient), jnp.float32)
    grad_rows[...] = gradient.T.astype(jnp.bfloat16)

    root_pair = forward(root_copies, root_all)
    for copy in root_pair:
        copy.wait_recv()
    locals_[1].wait()
    locals_[2].wait()
    for copy in grad_copies:
        copy.wait_recv()

    total = jnp.zeros((1, 1), jnp.float32)
    pre_copies = []
    for d in tuple(inner_steps) + (0,):
        block = inner_peer(d)
        acc = jnp.zeros((own_rows, cols), jnp.float32)
        for o in range(outer):
            acc = acc + dot(
                root_all[block, :, o * chunk : (o + 1) * chunk], grad_t[o], ((1,), (1,))
            )
        left_half = acc.astype(jnp.bfloat16)
        for k in range(heads_each):
            span = slice(k * size, (k + 1) * size)
            precond = dot(left_half[:, span], rr_ref[ij * heads_each + k], ((1,), (0,)))
            total = total + jnp.sum(precond * precond)
            pre_out[block, :, span] = precond.astype(jnp.bfloat16)
        if d:
            pre_copies.append(send(pre_out.at[block], pre_in.at[ij], inner_id(d)))
    pre_in[ij] = pre_out[ij]
    square_out[0, 1] = jnp.broadcast_to(total, (8, 128))
    square_copy = send(square_out.at[0], square_in.at[0], sibling)

    def stat_part(core_half, k):
        return dot(grad_rows[...], grad_t[core_half * (outer // 2) + k], ((1,), (0,)))

    for k in range(outer // 2):
        pair_out[:, k * chunk : (k + 1) * chunk] = stat_part(1 - core, k).astype(jnp.bfloat16)
    pair_copy = send(pair_out, pair_in, sibling)

    square_copy.wait_recv()
    square_out[1] = square_out[0] + square_in[0]
    square_copies = [
        send(square_out.at[1], square_in.at[d], inner_id(d)) for d in inner_steps
    ]
    for k in range(heads_each):
        product = jnp.zeros((size, size), jnp.float32)
        for o in range(outer):
            piece = grad_t[o, k * size : (k + 1) * size, :]
            product = product + dot(piece, piece, ((1,), (1,)))
        prod_all[ij, k] = product.astype(jnp.bfloat16)
    prod_copies = [send(prod_all.at[ij], prod_all.at[ij], inner_id(d)) for d in inner_steps]

    squares = square_out[1]
    for d, copy in zip(inner_steps, square_copies):
        copy.wait_recv()
        squares = squares + square_in[d]
    square_out[2] = squares
    square_copies = [
        send(square_out.at[2], square_in.at[inner + d - 1], outer_id(d)) for d in outer_steps
    ]
    for k in range(outer // 2):
        stat_own[:, k * chunk : (k + 1) * chunk] = stat_part(core, k)

    for copy in pre_copies:
        copy.wait_recv()
    locals_[3].wait()
    for d, copy in zip(outer_steps, square_copies):
        copy.wait_recv()
        squares = squares + square_in[inner + d - 1]
    factor = jnp.sqrt((squares[0] + epsilon) / (squares[1] + epsilon))[0:1, 0:1]

    def rows_of(o, j):
        return pl.ds(pl.multiple_of((o * inner + j) * own_rows, own_rows), own_rows)

    place = rows_of(oi, ij)
    for j in range(inner):
        span = slice(j * cols, (j + 1) * cols)
        step = factor * pre_in[j].astype(jnp.float32)
        updated = w_ref[:, span] - learn_rate * step
        step_ref[:, span] = step
        new_weight_ref[:, span] = updated
        copy_ref[place, span] = updated.astype(jnp.bfloat16)
    own = copy_ref.at[place, :]
    outer_copies = [send(own, own, outer_id(d)) for d in outer_steps]
    inner_copies = [send(own, own, inner_id(d)) for d in inner_steps]

    pair_copy.wait_recv()
    stat_copies = []
    for d in tuple(inner_steps) + (0,):
        span = pl.ds(pl.multiple_of(inner_peer(d) * own_rows, own_rows), own_rows)
        summed = stat_own[span, :] + pair_in[span, :].astype(jnp.float32)
        if d:
            stat_out[d - 1] = summed.astype(jnp.bfloat16)
            stat_copies.append(send(stat_out.at[d - 1], stat_in.at[d - 1], inner_id(d)))
        else:
            stat_sum = summed

    for d, copy in zip(outer_steps, outer_copies):
        copy.wait_recv()
        block = copy_ref.at[rows_of(lax.rem(oi + outer - d, outer), ij), :]
        inner_copies += [send(block, block, inner_id(e)) for e in inner_steps]

    for copy in prod_copies:
        copy.wait_recv()
    locals_[5].wait()
    for j in range(inner):
        for k in range(heads_each):
            h = j * heads_each + k
            new_right_ref[h] = decay_rate * rs_ref[h] + (1.0 - decay_rate) / width * prod_all[
                j, k
            ].astype(jnp.float32)
    locals_[4].wait()
    for copy in stat_copies:
        copy.wait_recv()
    for d in inner_steps:
        stat_sum = stat_sum + stat_in[d - 1].astype(jnp.float32)
    scale = (1.0 - decay_rate) / (2 * inner * cols)
    new_left_ref[...] = decay_rate * ls_ref[...] + scale * stat_sum
    for copy in inner_copies:
        copy.wait_recv()
    for copy in started:
        copy.wait_send()


def fused(
    cotangent,
    values_first,
    values_second,
    head_lambda,
    out_gain,
    weight,
    left_stat,
    right_stat,
    left_root,
    right_root,
):
    inner = INNER
    outer = lax.axis_size("fs") // inner
    rows, width = cotangent.shape
    own_rows, own_cols = weight.shape
    size = out_gain.shape[0]
    cols = own_cols // inner
    heads_each = cols // size
    chunk = width // outer
    half = width // 2
    group_rows = inner * own_rows
    bf16, f32 = jnp.bfloat16, jnp.float32
    vmem = pl.BlockSpec(memory_space=pltpu.VMEM)
    anywhere = pl.BlockSpec(memory_space=pl.ANY)
    copies = 11 * (inner - 1) + 4 * (outer - 1) + (outer - 1) * (inner - 1) + 2
    return pl.pallas_call(
        functools.partial(fused_kernel, outer, inner),
        out_shape=(
            jax.ShapeDtypeStruct(weight.shape, f32),
            jax.ShapeDtypeStruct(weight.shape, f32),
            jax.ShapeDtypeStruct((width, own_cols), bf16),
            jax.ShapeDtypeStruct(left_stat.shape, f32),
            jax.ShapeDtypeStruct(right_stat.shape, f32),
        ),
        in_specs=[pl.BlockSpec(memory_space=pltpu.SMEM)] + [vmem] * 5 + [anywhere] * 4,
        out_specs=[vmem] * 5,
        scratch_shapes=[
            pltpu.VMEM((inner, rows, width), bf16),
            pltpu.VMEM((inner, own_rows, width), bf16),
            pltpu.VMEM((inner, cols, rows), bf16),
            pltpu.VMEM((inner, cols, rows), bf16),
            pltpu.VMEM((outer - 1, cols, chunk), bf16),
            pltpu.VMEM((outer - 1, cols, chunk), bf16),
            pltpu.VMEM((outer, cols, chunk), bf16),
            pltpu.VMEM((chunk, cols), bf16),
            pltpu.VMEM((inner, own_rows, cols), bf16),
            pltpu.VMEM((inner, own_rows, cols), bf16),
            pltpu.VMEM((inner, heads_each, size, size), bf16),
            pltpu.VMEM((3, 2, 8, 128), f32),
            pltpu.VMEM((inner + outer - 1, 2, 8, 128), f32),
            pltpu.VMEM((group_rows, half), f32),
            pltpu.VMEM((group_rows, half), bf16),
            pltpu.VMEM((group_rows, half), bf16),
            pltpu.VMEM((inner - 1, own_rows, half), bf16),
            pltpu.VMEM((inner - 1, own_rows, half), bf16),
            pltpu.VMEM(right_root.shape, bf16),
            pltpu.VMEM(weight.shape, f32),
            pltpu.VMEM(left_stat.shape, f32),
            pltpu.VMEM(right_stat.shape, f32),
            pltpu.SemaphoreType.DMA((copies,)),
            pltpu.SemaphoreType.DMA((copies,)),
            pltpu.SemaphoreType.DMA((6,)),
        ],
        compiler_params=pltpu.CompilerParams(
            collective_id=0, has_side_effects=True, vmem_limit_bytes=56 * 1024 * 1024
        ),
        name="fused_update",
    )(
        head_lambda,
        cotangent,
        values_first,
        values_second,
        out_gain.reshape(1, size),
        left_root,
        right_root,
        weight,
        left_stat,
        right_stat,
    )


def step(*args):
    head_count, size = args[3].shape[0], args[4].shape[0]
    outer, rest = divmod(lax.axis_size("fs"), INNER)
    aligned = (
        rest == 0
        and lax.axis_size("tp") == 2
        and outer > 1
        and outer % 2 == 0
        and head_count % INNER == 0
        and size == 128
        and args[0].shape[0] % 128 == 0
        and args[5].shape[0] % 16 == 0
        and (args[0].shape[1] // outer) % 128 == 0
    )
    return tuple(fused(*args)) if aligned else shards(*args)


def solution(mesh):
    return jax.shard_map(
        step,
        mesh=mesh,
        in_specs=(
            P("fs", None),
            P("fs", "tp"),
            P("fs", "tp"),
            P("tp"),
            P(),
            P("fs", "tp"),
            P("fs", "tp"),
            P("tp", None, None),
            P("fs", None),
            P("tp", None, None),
        ),
        out_specs=(P("fs", "tp"), P("fs", "tp"), P(None, "tp"), P("fs", "tp"), P("tp", None, None)),
        check_vma=False,
    )
```

```python
import functools

import jax
import jax.numpy as jnp
from jax import lax
from jax.experimental import pallas as pl
from jax.experimental.pallas import tpu as pltpu
from jax.sharding import PartitionSpec as P

MESH = pl.DeviceIdType.MESH
INNER = 4

epsilon = 1e-06
decay_rate = 0.9
learn_rate = 0.01
output_scale = 0.2


def normalized(values_first, values_second, head_lambda, out_gain):
    token_count = values_first.shape[0]
    head_count = head_lambda.shape[0]
    head_size = out_gain.shape[0]
    first = values_first.astype(jnp.float32).reshape(token_count, head_count, head_size)
    second = values_second.astype(jnp.float32).reshape(token_count, head_count, head_size)
    difference = first - head_lambda[None, :, None] * second
    inverse = lax.rsqrt(jnp.mean(difference * difference, axis=-1, keepdims=True) + epsilon)
    scaled = difference * inverse * out_gain * output_scale
    return scaled.reshape(token_count, head_count * head_size).astype(jnp.bfloat16)


def by_head(matrix, head_count):
    return matrix.reshape(matrix.shape[0], head_count, matrix.shape[1] // head_count)


def head_products(matrix, head_count):
    heads = by_head(matrix, head_count)
    return jnp.einsum("rhi,rhj->hij", heads, heads, preferred_element_type=jnp.float32)


def shards(
    cotangent,
    values_first,
    values_second,
    head_lambda,
    out_gain,
    weight,
    left_stat,
    right_stat,
    left_root,
    right_root,
):
    head_count = head_lambda.shape[0]
    own_rows = weight.shape[0]
    own_cols = weight.shape[1]
    width = left_root.shape[1]
    total_cols = own_cols * lax.axis_size("tp")
    head_out = normalized(values_first, values_second, head_lambda, out_gain)
    contract_rows = (((0,), (0,)), ((), ()))
    contract_cols = (((1,), (1,)), ((), ()))
    gradient = lax.psum_scatter(
        lax.dot_general(cotangent, head_out, contract_rows, preferred_element_type=jnp.float32),
        "fs",
        scatter_dimension=0,
        tiled=True,
    )
    grad_half = gradient.astype(jnp.bfloat16)
    portion = lax.all_gather(grad_half, "fs", axis=0, tiled=True)
    left_acc = jnp.dot(left_root, portion, preferred_element_type=jnp.float32)
    products = lax.dot_general(
        grad_half, portion, contract_cols, preferred_element_type=jnp.float32
    )
    stat_cols = products
    right_acc = head_products(portion, head_count)
    left_acc, stat_cols, right_acc = (left_acc, stat_cols, right_acc)
    left_summed = lax.psum_scatter(
        stat_cols.astype(jnp.bfloat16), "tp", scatter_dimension=1, tiled=True
    ).astype(jnp.float32)
    new_left_stat = decay_rate * left_stat + (1.0 - decay_rate) / total_cols * left_summed
    new_right_stat = decay_rate * right_stat + (1.0 - decay_rate) / width * right_acc
    left_half = left_acc.astype(jnp.bfloat16)
    precond = jnp.einsum(
        "rhi,hij->rhj",
        by_head(left_half, head_count),
        right_root,
        preferred_element_type=jnp.float32,
    )
    precond = precond.reshape(own_rows, own_cols)
    grad_square, update_square = lax.psum(
        (jnp.sum(gradient * gradient), jnp.sum(precond * precond)), ("fs", "tp")
    )
    factor = jnp.sqrt((grad_square + epsilon) / (update_square + epsilon))
    update_step = factor * precond
    new_weight = weight - learn_rate * update_step
    new_copy = lax.all_gather(new_weight.astype(jnp.bfloat16), "fs", axis=0, tiled=True)
    return (update_step, new_weight, new_copy, new_left_stat, new_right_stat)


def dot(a, b, dims):
    return lax.dot_general(a, b, (dims, ((), ())), preferred_element_type=jnp.float32)


def fused_kernel(
    outer,
    inner,
    lam_ref,
    gain_ref,
    cot_hbm,
    first_hbm,
    second_hbm,
    root_hbm,
    right_root_hbm,
    weight_hbm,
    left_stat_hbm,
    right_stat_hbm,
    step_ref,
    new_weight_ref,
    copy_ref,
    new_left_ref,
    new_right_ref,
    cot_all,
    root_all,
    head_out,
    head_in,
    part_out,
    part_in,
    own_part,
    grad_t,
    grad_rows,
    pre_out,
    pre_in,
    prod_all,
    square_out,
    square_in,
    stat_own,
    pair_out,
    pair_in,
    stat_out,
    stat_in,
    first_ref,
    second_ref,
    rr_ref,
    w_ref,
    ls_ref,
    rs_ref,
    send_sem,
    recv_sem,
    local_sem,
):
    me = lax.axis_index("fs")
    core = lax.axis_index("tp")
    oi = me // inner
    ij = lax.rem(me, inner)
    rows, width = cot_hbm.shape
    own_rows = root_hbm.shape[0]
    size = gain_ref.shape[1]
    cols = head_in.shape[1]
    heads_each = cols // size
    chunk = width // outer
    half = width // 2
    mine = pl.ds(pl.multiple_of(core * half, half), half)

    def inner_peer(d):
        return lax.rem(ij + d, inner)

    is_mid = lax.rem((oi + 1) // 2, 2)
    near = oi + 1 - 2 * lax.rem(oi, 2)
    across = 2 - oi // 2
    far = (outer - 1) * (1 - oi // 2)
    x_peer = ij + 1 - 2 * lax.rem(ij, 2)
    y_peer = lax.rem(ij + 2, inner)

    def inner_id(d):
        return (oi * inner + inner_peer(d), core)

    def outer_id(o):
        return (o * inner + ij, core)

    def inner_at(j):
        return (oi * inner + j, core)

    sibling = (me, 1 - core)
    started = []
    started_mid = []
    used = [0]

    def fresh(count=1):
        used[0] += count
        return used[0] - count

    def describe(src, dst, device, arrival):
        return pltpu.make_async_remote_copy(
            src_ref=src,
            dst_ref=dst,
            send_sem=send_sem.at[fresh()],
            recv_sem=recv_sem.at[arrival],
            device_id=device,
            device_id_type=MESH,
        )

    arrivals = [0]

    def expect(count=1):
        arrivals[0] += count
        return arrivals[0] - count

    def send(src, dst, device, arrival=None):
        copy = describe(src, dst, device, expect() if arrival is None else arrival)
        copy.start()
        started.append(copy)
        return copy

    def arrived(ref, arrival):
        pltpu.make_async_copy(ref, ref, recv_sem.at[arrival]).wait()

    def gather_outer(block):
        base = expect(3)
        own = block(oi)
        send(own, own, outer_id(across), base + 1 + is_mid)
        direct = describe(own, own, outer_id(far), base + 2)
        relayed = describe(block(far), block(far), outer_id(near), base + 1)

        @pl.when(is_mid == 1)
        def _():
            direct.start()

        send(own, own, outer_id(near), base)
        started_mid.extend([direct, relayed])

        def wait_near():
            arrived(block(near), base)

        def wait_far():
            arrived(block(far), base + 1)

            @pl.when(is_mid == 1)
            def _():
                relayed.start()

        def wait_across():
            arrived(block(across), base + 2)

        return wait_near, wait_far, wait_across

    inner_steps = range(1, inner)
    outer_steps = range(1, outer)

    locals_ = [
        pltpu.make_async_copy(cot_hbm, cot_all.at[ij], local_sem.at[0]),
        pltpu.make_async_copy(root_hbm, root_all.at[ij], local_sem.at[1]),
        pltpu.make_async_copy(right_root_hbm, rr_ref, local_sem.at[2]),
        pltpu.make_async_copy(weight_hbm, w_ref, local_sem.at[3]),
        pltpu.make_async_copy(left_stat_hbm, ls_ref, local_sem.at[4]),
        pltpu.make_async_copy(right_stat_hbm, rs_ref, local_sem.at[5]),
        pltpu.make_async_copy(first_hbm, first_ref, local_sem.at[6]),
        pltpu.make_async_copy(second_hbm, second_ref, local_sem.at[7]),
    ]
    for index in (0, 6, 7, 1, 2, 3, 4, 5):
        locals_[index].start()

    barrier = pltpu.get_barrier_semaphore()
    peers = [inner_id(d) for d in inner_steps] + [outer_id(lax.rem(oi + d, outer)) for d in outer_steps] + [sibling]
    for peer in peers:
        pl.semaphore_signal(barrier, inc=1, device_id=peer, device_id_type=MESH)
    pl.semaphore_wait(barrier, len(peers))

    locals_[0].wait()
    own_cot = cot_all.at[ij, :, mine]
    cot_copies = [send(own_cot, own_cot, inner_id(d)) for d in inner_steps]
    locals_[6].wait()
    locals_[7].wait()

    gain = gain_ref[...] * output_scale
    for h in range(inner * heads_each):
        span = slice(h * size, (h + 1) * size)
        first = first_ref[:, span].astype(jnp.float32)
        second = second_ref[:, span].astype(jnp.float32)
        difference = first - lam_ref[h] * second
        inverse = lax.rsqrt(jnp.mean(difference * difference, axis=-1, keepdims=True) + epsilon)
        scaled = difference * inverse * gain
        k = h % heads_each
        head_out[h // heads_each, k * size : (k + 1) * size, :] = scaled.T.astype(jnp.bfloat16)
    head_copies = [
        send(head_out.at[inner_peer(d)], head_in.at[ij], inner_id(d)) for d in inner_steps
    ]
    head_in[ij] = head_out[ij]

    def forward(copies, buffer):
        result = []
        for d, copy in zip(inner_steps, copies):
            copy.wait_recv()
            place = buffer.at[lax.rem(ij + inner - d, inner), :, mine]
            result.append(send(place, place, sibling))
        return result

    cot_pair = forward(cot_copies, cot_all)
    for copy in head_copies:
        copy.wait_recv()
    locals_[1].wait()
    own_root = root_all.at[ij, :, mine]
    root_copies = [send(own_root, own_root, inner_id(d)) for d in inner_steps]
    for copy in cot_pair:
        copy.wait_recv()

    lhs = jnp.concatenate([head_in[j] for j in range(inner)], axis=1)

    def part(owner):
        span = pl.ds(pl.multiple_of(owner * chunk, chunk), chunk)
        rhs = cot_all[:, :, span].reshape(inner * rows, chunk)
        return dot(lhs, rhs, ((1,), (0,)))

    base = expect(4)
    part_out[0] = part(far).astype(jnp.bfloat16)
    to_relay = describe(part_out.at[0], part_in.at[3], outer_id(near), base + 3)

    @pl.when(is_mid == 0)
    def _():
        to_relay.start()

    part_out[1] = part(across).astype(jnp.bfloat16)
    slot = 2 - is_mid
    send(part_out.at[1], part_in.at[slot], outer_id(across), base + slot)
    part_out[2] = part(near).astype(jnp.bfloat16)
    send(part_out.at[2], part_in.at[0], outer_id(near), base)
    combined = describe(part_out.at[3], part_in.at[1], outer_id(far), base + 1)

    @pl.when(is_mid == 1)
    def _():
        arrived(part_in.at[3], base + 3)
        total_far = part(far) + part_in[3].astype(jnp.float32)
        part_out[3] = total_far.astype(jnp.bfloat16)
        combined.start()

    own_part[...] = part(oi)
    arrived(part_in.at[0], base)
    own_part[...] += part_in[0].astype(jnp.float32)

    @pl.when(is_mid == 1)
    def _():
        arrived(part_in.at[2], base + 2)
        own_part[...] += part_in[2].astype(jnp.float32)

    arrived(part_in.at[1], base + 1)
    gradient = own_part[...] + part_in[1].astype(jnp.float32)
    grad_t[oi] = gradient.astype(jnp.bfloat16)
    wait_near, wait_far, wait_across = gather_outer(lambda o: grad_t.at[o])
    square_out[0, 0] = jnp.full((8, 128), jnp.sum(gradient * gradient), jnp.float32)
    grad_rows[...] = gradient.T.astype(jnp.bfloat16)

    root_pair = forward(root_copies, root_all)
    wait_far()
    for copy in root_pair:
        copy.wait_recv()
    locals_[2].wait()
    wait_near()
    wait_across()

    total = jnp.zeros((1, 1), jnp.float32)
    pre_copies = []
    for d in tuple(inner_steps) + (0,):
        block = inner_peer(d)
        acc = jnp.zeros((own_rows, cols), jnp.float32)
        for o in range(outer):
            acc = acc + dot(
                root_all[block, :, o * chunk : (o + 1) * chunk], grad_t[o], ((1,), (1,))
            )
        left_half = acc.astype(jnp.bfloat16)
        for k in range(heads_each):
            span = slice(k * size, (k + 1) * size)
            precond = dot(left_half[:, span], rr_ref[ij * heads_each + k], ((1,), (0,)))
            total = total + jnp.sum(precond * precond)
            pre_out[block, :, span] = precond.astype(jnp.bfloat16)
        if d:
            pre_copies.append(send(pre_out.at[block], pre_in.at[ij], inner_id(d)))
    pre_in[ij] = pre_out[ij]
    square_out[0, 1] = jnp.broadcast_to(total, (8, 128))
    square_copy = send(square_out.at[0], square_in.at[0], sibling)

    def stat_part(core_half, k):
        return dot(grad_rows[...], grad_t[core_half * (outer // 2) + k], ((1,), (0,)))

    for k in range(outer // 2):
        pair_out[:, k * chunk : (k + 1) * chunk] = stat_part(1 - core, k).astype(jnp.bfloat16)
    pair_copy = send(pair_out, pair_in, sibling)

    square_copy.wait_recv()
    square_out[1] = square_out[0] + square_in[0]
    square_copies = [
        send(square_out.at[1], square_in.at[d], inner_id(d)) for d in inner_steps
    ]
    for k in range(heads_each):
        product = jnp.zeros((size, size), jnp.float32)
        for o in range(outer):
            piece = grad_t[o, k * size : (k + 1) * size, :]
            product = product + dot(piece, piece, ((1,), (1,)))
        prod_all[ij, k] = product.astype(jnp.bfloat16)
    prod_copies = [send(prod_all.at[ij], prod_all.at[ij], inner_id(d)) for d in inner_steps]

    squares = square_out[1]
    for d, copy in zip(inner_steps, square_copies):
        copy.wait_recv()
        squares = squares + square_in[d]
    square_out[2] = squares
    square_copies = [
        send(
            square_out.at[2],
            square_in.at[inner + d - 1],
            outer_id(lax.rem(oi + d, outer)),
        )
        for d in outer_steps
    ]
    for k in range(outer // 2):
        stat_own[:, k * chunk : (k + 1) * chunk] = stat_part(core, k)

    pair_copy.wait_recv()
    stat_copies = []
    for d in tuple(inner_steps) + (0,):
        span = pl.ds(pl.multiple_of(inner_peer(d) * own_rows, own_rows), own_rows)
        summed = stat_own[span, :] + pair_in[span, :].astype(jnp.float32)
        if d:
            stat_out[d - 1] = summed.astype(jnp.bfloat16)
            stat_copies.append(send(stat_out.at[d - 1], stat_in.at[d - 1], inner_id(d)))
        else:
            stat_own[span, :] = summed

    for copy in pre_copies:
        copy.wait_recv()
    locals_[3].wait()
    for d, copy in zip(outer_steps, square_copies):
        copy.wait_recv()
        squares = squares + square_in[inner + d - 1]
    factor = jnp.sqrt((squares[0] + epsilon) / (squares[1] + epsilon))[0:1, 0:1]

    def rows_of(o, j):
        return pl.ds(pl.multiple_of((o * inner + j) * own_rows, own_rows), own_rows)

    place = rows_of(oi, ij)
    for j in range(inner):
        span = slice(j * cols, (j + 1) * cols)
        step = factor * pre_in[j].astype(jnp.float32)
        updated = w_ref[:, span] - learn_rate * step
        step_ref[:, span] = step
        new_weight_ref[:, span] = updated
        copy_ref[place, span] = updated.astype(jnp.bfloat16)
    near_in, far_in, across_in = gather_outer(lambda o: copy_ref.at[rows_of(o, ij), :])

    def halves(o, j):
        start = (o * inner + j) * own_rows
        return [
            copy_ref.at[pl.ds(pl.multiple_of(start + k * (own_rows // 2), own_rows // 2), own_rows // 2), :]
            for k in range(2)
        ]

    flight = []

    def spread(o):
        block = copy_ref.at[rows_of(o, ij), :]
        flight.append((o, send(block, block, inner_at(x_peer)), send(block, block, inner_at(y_peer))))

    last = []

    def pass_on(index):
        o, from_x, from_y = flight[index]
        from_x.wait_recv()
        piece = halves(o, x_peer)[0]
        last.append(send(piece, piece, inner_at(y_peer)))
        from_y.wait_recv()
        piece = halves(o, y_peer)[1]
        last.append(send(piece, piece, inner_at(x_peer)))

    spread(oi)
    near_in()
    spread(near)
    pass_on(0)
    far_in()
    across_in()
    spread(across)
    pass_on(1)
    spread(far)
    pass_on(2)
    pass_on(3)

    for copy in prod_copies:
        copy.wait_recv()
    locals_[5].wait()
    for j in range(inner):
        for k in range(heads_each):
            h = j * heads_each + k
            new_right_ref[h] = decay_rate * rs_ref[h] + (1.0 - decay_rate) / width * prod_all[
                j, k
            ].astype(jnp.float32)
    locals_[4].wait()
    for copy in stat_copies:
        copy.wait_recv()
    stat_sum = stat_own[pl.ds(pl.multiple_of(ij * own_rows, own_rows), own_rows), :]
    for d in inner_steps:
        stat_sum = stat_sum + stat_in[d - 1].astype(jnp.float32)
    scale = (1.0 - decay_rate) / (2 * inner * cols)
    new_left_ref[...] = decay_rate * ls_ref[...] + scale * stat_sum
    for copy in last:
        copy.wait_recv()
    for copy in started:
        copy.wait_send()

    @pl.when(is_mid == 1)
    def _():
        combined.wait_send()
        for copy in started_mid:
            copy.wait_send()

    @pl.when(is_mid == 0)
    def _():
        to_relay.wait_send()


def fused(
    cotangent,
    values_first,
    values_second,
    head_lambda,
    out_gain,
    weight,
    left_stat,
    right_stat,
    left_root,
    right_root,
):
    inner = INNER
    outer = lax.axis_size("fs") // inner
    rows, width = cotangent.shape
    own_rows, own_cols = weight.shape
    size = out_gain.shape[0]
    cols = own_cols // inner
    heads_each = cols // size
    chunk = width // outer
    half = width // 2
    group_rows = inner * own_rows
    bf16, f32 = jnp.bfloat16, jnp.float32
    vmem = pl.BlockSpec(memory_space=pltpu.VMEM)
    anywhere = pl.BlockSpec(memory_space=pl.ANY)
    copies = 12 * inner + 5 * outer + 4 * outer
    return pl.pallas_call(
        functools.partial(fused_kernel, outer, inner),
        out_shape=(
            pltpu.VMEM(weight.shape, f32),
            pltpu.VMEM(weight.shape, f32),
            pltpu.VMEM((width, own_cols), bf16),
            pltpu.VMEM(left_stat.shape, f32),
            pltpu.VMEM(right_stat.shape, f32),
        ),
        in_specs=[pl.BlockSpec(memory_space=pltpu.SMEM)] + [vmem] + [anywhere] * 8,
        out_specs=[vmem] * 5,
        scratch_shapes=[
            pltpu.VMEM((inner, rows, width), bf16),
            pltpu.VMEM((inner, own_rows, width), bf16),
            pltpu.VMEM((inner, cols, rows), bf16),
            pltpu.VMEM((inner, cols, rows), bf16),
            pltpu.VMEM((outer, cols, chunk), bf16),
            pltpu.VMEM((outer, cols, chunk), bf16),
            pltpu.VMEM((cols, chunk), f32),
            pltpu.VMEM((outer, cols, chunk), bf16),
            pltpu.VMEM((chunk, cols), bf16),
            pltpu.VMEM((inner, own_rows, cols), bf16),
            pltpu.VMEM((inner, own_rows, cols), bf16),
            pltpu.VMEM((inner, heads_each, size, size), bf16),
            pltpu.VMEM((3, 2, 8, 128), f32),
            pltpu.VMEM((inner + outer - 1, 2, 8, 128), f32),
            pltpu.VMEM((group_rows, half), f32),
            pltpu.VMEM((group_rows, half), bf16),
            pltpu.VMEM((group_rows, half), bf16),
            pltpu.VMEM((inner - 1, own_rows, half), bf16),
            pltpu.VMEM((inner - 1, own_rows, half), bf16),
            pltpu.VMEM(values_first.shape, bf16),
            pltpu.VMEM(values_second.shape, bf16),
            pltpu.VMEM(right_root.shape, bf16),
            pltpu.VMEM(weight.shape, f32),
            pltpu.VMEM(left_stat.shape, f32),
            pltpu.VMEM(right_stat.shape, f32),
            pltpu.SemaphoreType.DMA((copies,)),
            pltpu.SemaphoreType.DMA((copies,)),
            pltpu.SemaphoreType.DMA((8,)),
        ],
        compiler_params=pltpu.CompilerParams(
            collective_id=0, has_side_effects=True, vmem_limit_bytes=56 * 1024 * 1024
        ),
        name="fused_update",
    )(
        head_lambda,
        out_gain.reshape(1, size),
        cotangent,
        values_first,
        values_second,
        left_root,
        right_root,
        weight,
        left_stat,
        right_stat,
    )


def step(*args):
    head_count, size = args[3].shape[0], args[4].shape[0]
    outer, rest = divmod(lax.axis_size("fs"), INNER)
    aligned = (
        rest == 0
        and lax.axis_size("tp") == 2
        and outer == 4
        and head_count % INNER == 0
        and size == 128
        and args[0].shape[0] % 128 == 0
        and args[5].shape[0] % 16 == 0
        and (args[0].shape[1] // outer) % 128 == 0
    )
    return tuple(fused(*args)) if aligned else shards(*args)


def solution(mesh):
    return jax.shard_map(
        step,
        mesh=mesh,
        in_specs=(
            P("fs", None),
            P("fs", "tp"),
            P("fs", "tp"),
            P("tp"),
            P(),
            P("fs", "tp"),
            P("fs", "tp"),
            P("tp", None, None),
            P("fs", None),
            P("tp", None, None),
        ),
        out_specs=(P("fs", "tp"), P("fs", "tp"), P(None, "tp"), P("fs", "tp"), P("tp", None, None)),
        check_vma=False,
    )
```

```python
import functools

import jax
import jax.numpy as jnp
from jax import lax
from jax.experimental import pallas as pl
from jax.experimental.pallas import tpu as pltpu
from jax.sharding import PartitionSpec as P

MESH = pl.DeviceIdType.MESH
INNER = 4

epsilon = 1e-06
decay_rate = 0.9
learn_rate = 0.01
output_scale = 0.2


def normalized(values_first, values_second, head_lambda, out_gain):
    token_count = values_first.shape[0]
    head_count = head_lambda.shape[0]
    head_size = out_gain.shape[0]
    first = values_first.astype(jnp.float32).reshape(token_count, head_count, head_size)
    second = values_second.astype(jnp.float32).reshape(token_count, head_count, head_size)
    difference = first - head_lambda[None, :, None] * second
    inverse = lax.rsqrt(jnp.mean(difference * difference, axis=-1, keepdims=True) + epsilon)
    scaled = difference * inverse * out_gain * output_scale
    return scaled.reshape(token_count, head_count * head_size).astype(jnp.bfloat16)


def by_head(matrix, head_count):
    return matrix.reshape(matrix.shape[0], head_count, matrix.shape[1] // head_count)


def head_products(matrix, head_count):
    heads = by_head(matrix, head_count)
    return jnp.einsum("rhi,rhj->hij", heads, heads, preferred_element_type=jnp.float32)


def shards(
    cotangent,
    values_first,
    values_second,
    head_lambda,
    out_gain,
    weight,
    left_stat,
    right_stat,
    left_root,
    right_root,
):
    head_count = head_lambda.shape[0]
    own_rows = weight.shape[0]
    own_cols = weight.shape[1]
    width = left_root.shape[1]
    total_cols = own_cols * lax.axis_size("tp")
    head_out = normalized(values_first, values_second, head_lambda, out_gain)
    contract_rows = (((0,), (0,)), ((), ()))
    contract_cols = (((1,), (1,)), ((), ()))
    gradient = lax.psum_scatter(
        lax.dot_general(cotangent, head_out, contract_rows, preferred_element_type=jnp.float32),
        "fs",
        scatter_dimension=0,
        tiled=True,
    )
    grad_half = gradient.astype(jnp.bfloat16)
    portion = lax.all_gather(grad_half, "fs", axis=0, tiled=True)
    left_acc = jnp.dot(left_root, portion, preferred_element_type=jnp.float32)
    products = lax.dot_general(
        grad_half, portion, contract_cols, preferred_element_type=jnp.float32
    )
    stat_cols = products
    right_acc = head_products(portion, head_count)
    left_acc, stat_cols, right_acc = (left_acc, stat_cols, right_acc)
    left_summed = lax.psum_scatter(
        stat_cols.astype(jnp.bfloat16), "tp", scatter_dimension=1, tiled=True
    ).astype(jnp.float32)
    new_left_stat = decay_rate * left_stat + (1.0 - decay_rate) / total_cols * left_summed
    new_right_stat = decay_rate * right_stat + (1.0 - decay_rate) / width * right_acc
    left_half = left_acc.astype(jnp.bfloat16)
    precond = jnp.einsum(
        "rhi,hij->rhj",
        by_head(left_half, head_count),
        right_root,
        preferred_element_type=jnp.float32,
    )
    precond = precond.reshape(own_rows, own_cols)
    grad_square, update_square = lax.psum(
        (jnp.sum(gradient * gradient), jnp.sum(precond * precond)), ("fs", "tp")
    )
    factor = jnp.sqrt((grad_square + epsilon) / (update_square + epsilon))
    update_step = factor * precond
    new_weight = weight - learn_rate * update_step
    new_copy = lax.all_gather(new_weight.astype(jnp.bfloat16), "fs", axis=0, tiled=True)
    return (update_step, new_weight, new_copy, new_left_stat, new_right_stat)


def dot(a, b, dims):
    return lax.dot_general(a, b, (dims, ((), ())), preferred_element_type=jnp.float32)


def fused_kernel(
    outer,
    inner,
    lam_ref,
    gain_ref,
    cot_hbm,
    first_hbm,
    second_hbm,
    root_hbm,
    right_root_hbm,
    weight_hbm,
    left_stat_hbm,
    right_stat_hbm,
    step_ref,
    new_weight_ref,
    copy_ref,
    new_left_ref,
    new_right_ref,
    cot_all,
    root_all,
    head_out,
    head_in,
    part_out,
    part_in,
    own_part,
    grad_t,
    grad_rows,
    pre_out,
    pre_in,
    prod_all,
    square_out,
    square_in,
    stat_own,
    pair_out,
    pair_in,
    stat_out,
    stat_in,
    first_ref,
    second_ref,
    rr_ref,
    w_ref,
    ls_ref,
    rs_ref,
    send_sem,
    recv_sem,
    local_sem,
):
    me = lax.axis_index("fs")
    core = lax.axis_index("tp")
    oi = me // inner
    ij = lax.rem(me, inner)
    rows, width = cot_hbm.shape
    own_rows = root_hbm.shape[0]
    size = gain_ref.shape[1]
    cols = head_in.shape[1]
    heads_each = cols // size
    chunk = width // outer
    half = width // 2
    mine = pl.ds(pl.multiple_of(core * half, half), half)

    def inner_peer(d):
        return lax.rem(ij + d, inner)

    is_mid = lax.rem((oi + 1) // 2, 2)
    near = oi + 1 - 2 * lax.rem(oi, 2)
    across = 2 - oi // 2
    far = (outer - 1) * (1 - oi // 2)
    x_peer = ij + 1 - 2 * lax.rem(ij, 2)
    y_peer = lax.rem(ij + 2, inner)

    def inner_id(d):
        return (oi * inner + inner_peer(d), core)

    def outer_id(o):
        return (o * inner + ij, core)

    def inner_at(j):
        return (oi * inner + j, core)

    sibling = (me, 1 - core)
    started = []
    started_mid = []
    used = [0]

    def fresh(count=1):
        used[0] += count
        return used[0] - count

    def describe(src, dst, device, arrival):
        return pltpu.make_async_remote_copy(
            src_ref=src,
            dst_ref=dst,
            send_sem=send_sem.at[fresh()],
            recv_sem=recv_sem.at[arrival],
            device_id=device,
            device_id_type=MESH,
        )

    arrivals = [0]

    def expect(count=1):
        arrivals[0] += count
        return arrivals[0] - count

    def send(src, dst, device, arrival=None):
        copy = describe(src, dst, device, expect() if arrival is None else arrival)
        copy.start()
        started.append(copy)
        return copy

    def arrived(ref, arrival):
        pltpu.make_async_copy(ref, ref, recv_sem.at[arrival]).wait()

    def gather_outer(block):
        base = expect(3)
        own = block(oi)
        send(own, own, outer_id(across), base + 1 + is_mid)
        direct = describe(own, own, outer_id(far), base + 2)
        relayed = describe(block(far), block(far), outer_id(near), base + 1)

        @pl.when(is_mid == 1)
        def _():
            direct.start()

        send(own, own, outer_id(near), base)
        started_mid.extend([direct, relayed])

        def wait_near():
            arrived(block(near), base)

        def wait_far():
            arrived(block(far), base + 1)

            @pl.when(is_mid == 1)
            def _():
                relayed.start()

        def wait_across():
            arrived(block(across), base + 2)

        return wait_near, wait_far, wait_across

    inner_steps = range(1, inner)
    outer_steps = range(1, outer)

    locals_ = [
        pltpu.make_async_copy(cot_hbm, cot_all.at[ij], local_sem.at[0]),
        pltpu.make_async_copy(root_hbm, root_all.at[ij], local_sem.at[1]),
        pltpu.make_async_copy(right_root_hbm, rr_ref, local_sem.at[2]),
        pltpu.make_async_copy(weight_hbm, w_ref, local_sem.at[3]),
        pltpu.make_async_copy(left_stat_hbm, ls_ref, local_sem.at[4]),
        pltpu.make_async_copy(right_stat_hbm, rs_ref, local_sem.at[5]),
        pltpu.make_async_copy(first_hbm, first_ref, local_sem.at[6]),
        pltpu.make_async_copy(second_hbm, second_ref, local_sem.at[7]),
    ]
    for index in (0, 6, 7, 1, 2, 3, 4, 5):
        locals_[index].start()

    barrier = pltpu.get_barrier_semaphore()
    peers = [inner_id(d) for d in inner_steps] + [outer_id(lax.rem(oi + d, outer)) for d in outer_steps] + [sibling]
    for peer in peers:
        pl.semaphore_signal(barrier, inc=1, device_id=peer, device_id_type=MESH)
    pl.semaphore_wait(barrier, len(peers))

    locals_[0].wait()
    own_cot = cot_all.at[ij, :, mine]
    cot_copies = [send(own_cot, own_cot, inner_id(d)) for d in inner_steps]
    locals_[6].wait()
    locals_[7].wait()

    gain = gain_ref[...] * output_scale
    for h in range(inner * heads_each):
        span = slice(h * size, (h + 1) * size)
        first = first_ref[:, span].astype(jnp.float32)
        second = second_ref[:, span].astype(jnp.float32)
        difference = first - lam_ref[h] * second
        inverse = lax.rsqrt(jnp.mean(difference * difference, axis=-1, keepdims=True) + epsilon)
        scaled = difference * inverse * gain
        k = h % heads_each
        head_out[h // heads_each, k * size : (k + 1) * size, :] = scaled.T.astype(jnp.bfloat16)
    head_copies = [
        send(head_out.at[inner_peer(d)], head_in.at[ij], inner_id(d)) for d in inner_steps
    ]
    head_in[ij] = head_out[ij]

    def forward(copies, buffer):
        result = []
        for d, copy in zip(inner_steps, copies):
            copy.wait_recv()
            place = buffer.at[lax.rem(ij + inner - d, inner), :, mine]
            result.append(send(place, place, sibling))
        return result

    cot_pair = forward(cot_copies, cot_all)
    for copy in head_copies:
        copy.wait_recv()
    locals_[1].wait()
    own_root = root_all.at[ij, :, mine]
    root_copies = [send(own_root, own_root, inner_id(d)) for d in inner_steps]
    for copy in cot_pair:
        copy.wait_recv()

    def head(k):
        return slice(k * size, (k + 1) * size)

    heads = range(heads_each)
    lhs = [jnp.concatenate([head_in[j, head(k), :] for j in range(inner)], axis=1) for k in heads]

    def part(owner, k):
        span = pl.ds(pl.multiple_of(owner * chunk, chunk), chunk)
        rhs = cot_all[:, :, span].reshape(inner * rows, chunk)
        return dot(lhs[k], rhs, ((1,), (0,)))

    slot = 2 - is_mid
    bases, to_relay, combined = [], [], []
    for k in heads:
        base = expect(4)
        bases.append(base)
        part_out[k, 0] = part(far, k).astype(jnp.bfloat16)
        copy = describe(part_out.at[k, 0], part_in.at[k, 3], outer_id(near), base + 3)
        to_relay.append(copy)

        @pl.when(is_mid == 0)
        def _():
            copy.start()

        part_out[k, 1] = part(across, k).astype(jnp.bfloat16)
        send(part_out.at[k, 1], part_in.at[k, slot], outer_id(across), base + slot)
        part_out[k, 2] = part(near, k).astype(jnp.bfloat16)
        send(part_out.at[k, 2], part_in.at[k, 0], outer_id(near), base)
    for k in heads:
        copy = describe(part_out.at[k, 3], part_in.at[k, 1], outer_id(far), bases[k] + 1)
        combined.append(copy)

        @pl.when(is_mid == 1)
        def _():
            arrived(part_in.at[k, 3], bases[k] + 3)
            total_far = part_out[k, 0].astype(jnp.float32) + part_in[k, 3].astype(jnp.float32)
            part_out[k, 3] = total_far.astype(jnp.bfloat16)
            copy.start()

    for k in heads:
        own_part[k] = part(oi, k)
    grad_square = jnp.zeros((), jnp.float32)
    grad_waits = []
    for k in heads:
        base = bases[k]
        arrived(part_in.at[k, 0], base)
        own_part[k] += part_in[k, 0].astype(jnp.float32)

        @pl.when(is_mid == 1)
        def _():
            arrived(part_in.at[k, 2], base + 2)
            own_part[k] += part_in[k, 2].astype(jnp.float32)

        arrived(part_in.at[k, 1], base + 1)
        gradient = own_part[k] + part_in[k, 1].astype(jnp.float32)
        own_part[k] = gradient
        grad_t[oi, head(k), :] = gradient.astype(jnp.bfloat16)
        grad_waits.append(gather_outer(lambda o, k=k: grad_t.at[o, head(k), :]))
    for k in heads:
        gradient = own_part[k]
        grad_square = grad_square + jnp.sum(gradient * gradient)
        grad_rows[:, head(k)] = gradient.T.astype(jnp.bfloat16)
    square_out[0, 0] = jnp.full((8, 128), grad_square, jnp.float32)

    root_pair = forward(root_copies, root_all)
    grad_waits[0][1]()
    for copy in root_pair:
        copy.wait_recv()
    locals_[2].wait()

    total = jnp.zeros((1, 1), jnp.float32)
    for k in heads:
        wait_near, wait_far, wait_across = grad_waits[k]
        wait_near()
        wait_across()
        if k + 1 < heads_each:
            grad_waits[k + 1][1]()
        acc = jnp.zeros((inner * own_rows, size), jnp.float32)
        for o in range(outer):
            block = root_all[:, :, o * chunk : (o + 1) * chunk].reshape(inner * own_rows, chunk)
            acc = acc + dot(block, grad_t[o, head(k), :], ((1,), (1,)))
        precond = dot(acc.astype(jnp.bfloat16), rr_ref[ij * heads_each + k], ((1,), (0,)))
        total = total + jnp.sum(precond * precond)
        for j in range(inner):
            pre_out[j, :, head(k)] = precond[j * own_rows : (j + 1) * own_rows].astype(jnp.bfloat16)
    pre_copies = [send(pre_out.at[inner_peer(d)], pre_in.at[ij], inner_id(d)) for d in inner_steps]
    pre_in[ij] = pre_out[ij]
    square_out[0, 1] = jnp.broadcast_to(total, (8, 128))
    square_copy = send(square_out.at[0], square_in.at[0], sibling)

    def stat_part(core_half, k):
        return dot(grad_rows[...], grad_t[core_half * (outer // 2) + k], ((1,), (0,)))

    for k in range(outer // 2):
        pair_out[:, k * chunk : (k + 1) * chunk] = stat_part(1 - core, k).astype(jnp.bfloat16)
    pair_copy = send(pair_out, pair_in, sibling)

    square_copy.wait_recv()
    square_out[1] = square_out[0] + square_in[0]
    square_copies = [
        send(square_out.at[1], square_in.at[d], inner_id(d)) for d in inner_steps
    ]
    for k in range(heads_each):
        product = jnp.zeros((size, size), jnp.float32)
        for o in range(outer):
            piece = grad_t[o, k * size : (k + 1) * size, :]
            product = product + dot(piece, piece, ((1,), (1,)))
        prod_all[ij, k] = product.astype(jnp.bfloat16)
    prod_copies = [send(prod_all.at[ij], prod_all.at[ij], inner_id(d)) for d in inner_steps]

    squares = square_out[1]
    for d, copy in zip(inner_steps, square_copies):
        copy.wait_recv()
        squares = squares + square_in[d]
    square_out[2] = squares
    square_copies = [
        send(
            square_out.at[2],
            square_in.at[inner + d - 1],
            outer_id(lax.rem(oi + d, outer)),
        )
        for d in outer_steps
    ]
    for k in range(outer // 2):
        stat_own[:, k * chunk : (k + 1) * chunk] = stat_part(core, k)

    pair_copy.wait_recv()
    stat_copies = []
    for d in tuple(inner_steps) + (0,):
        span = pl.ds(pl.multiple_of(inner_peer(d) * own_rows, own_rows), own_rows)
        summed = stat_own[span, :] + pair_in[span, :].astype(jnp.float32)
        if d:
            stat_out[d - 1] = summed.astype(jnp.bfloat16)
            stat_copies.append(send(stat_out.at[d - 1], stat_in.at[d - 1], inner_id(d)))
        else:
            stat_own[span, :] = summed

    for copy in pre_copies:
        copy.wait_recv()
    locals_[3].wait()
    for d, copy in zip(outer_steps, square_copies):
        copy.wait_recv()
        squares = squares + square_in[inner + d - 1]
    factor = jnp.sqrt((squares[0] + epsilon) / (squares[1] + epsilon))[0:1, 0:1]

    def rows_of(o, j):
        return pl.ds(pl.multiple_of((o * inner + j) * own_rows, own_rows), own_rows)

    place = rows_of(oi, ij)
    for j in range(inner):
        span = slice(j * cols, (j + 1) * cols)
        step = factor * pre_in[j].astype(jnp.float32)
        updated = w_ref[:, span] - learn_rate * step
        step_ref[:, span] = step
        new_weight_ref[:, span] = updated
        copy_ref[place, span] = updated.astype(jnp.bfloat16)
    main = own_rows * 3 // 4
    rest = own_rows - main

    def piece(o, j, start, count):
        place = (o * inner + j) * own_rows + start
        return copy_ref.at[pl.ds(pl.multiple_of(place, own_rows // 8), count), :]

    last = []

    def spread(o, start, count):
        block = piece(o, ij, start, count)
        to_x = send(block, block, inner_at(x_peer))
        to_y = send(block, block, inner_at(y_peer))
        return o, start, count, to_x, to_y

    def pass_on(flight):
        o, start, count, from_x, from_y = flight
        part_rows = count // 2
        from_x.wait_recv()
        block = piece(o, x_peer, start, part_rows)
        one = send(block, block, inner_at(y_peer))
        from_y.wait_recv()
        block = piece(o, y_peer, start + part_rows, part_rows)
        return one, send(block, block, inner_at(x_peer))

    def gather_rest(j):
        return gather_outer(lambda o: piece(o, j, main, rest))

    rest_flight = spread(oi, main, rest)
    near_in, far_in, across_in = gather_outer(lambda o: piece(o, ij, 0, main))
    flight = spread(oi, 0, main)
    rest_waits = [gather_rest(ij)]
    rest_last = pass_on(rest_flight)
    rest_waits += [gather_rest(x_peer), gather_rest(y_peer)]
    near_in()
    near_flight = spread(near, 0, main)
    far_in()
    last += pass_on(flight)
    for copy in rest_last:
        copy.wait_recv()
    rest_waits.append(gather_rest(inner - 1 - ij))
    across_in()
    across_flight = spread(across, 0, main)
    rest_waits[0][1]()
    far_flight = spread(far, 0, main)
    last += pass_on(near_flight)
    rest_waits[1][1]()
    rest_waits[2][1]()
    last += pass_on(across_flight)
    rest_waits[3][1]()
    last += pass_on(far_flight)

    for copy in prod_copies:
        copy.wait_recv()
    locals_[5].wait()
    for j in range(inner):
        for k in range(heads_each):
            h = j * heads_each + k
            new_right_ref[h] = decay_rate * rs_ref[h] + (1.0 - decay_rate) / width * prod_all[
                j, k
            ].astype(jnp.float32)
    locals_[4].wait()
    for copy in stat_copies:
        copy.wait_recv()
    stat_sum = stat_own[pl.ds(pl.multiple_of(ij * own_rows, own_rows), own_rows), :]
    for d in inner_steps:
        stat_sum = stat_sum + stat_in[d - 1].astype(jnp.float32)
    scale = (1.0 - decay_rate) / (2 * inner * cols)
    new_left_ref[...] = decay_rate * ls_ref[...] + scale * stat_sum
    for copy in last:
        copy.wait_recv()
    for near_in, _, across_in in rest_waits:
        near_in()
        across_in()
    for copy in started:
        copy.wait_send()

    @pl.when(is_mid == 1)
    def _():
        for copy in combined + started_mid:
            copy.wait_send()

    @pl.when(is_mid == 0)
    def _():
        for copy in to_relay:
            copy.wait_send()


def fused(
    cotangent,
    values_first,
    values_second,
    head_lambda,
    out_gain,
    weight,
    left_stat,
    right_stat,
    left_root,
    right_root,
):
    inner = INNER
    outer = lax.axis_size("fs") // inner
    rows, width = cotangent.shape
    own_rows, own_cols = weight.shape
    size = out_gain.shape[0]
    cols = own_cols // inner
    heads_each = cols // size
    chunk = width // outer
    half = width // 2
    group_rows = inner * own_rows
    bf16, f32 = jnp.bfloat16, jnp.float32
    vmem = pl.BlockSpec(memory_space=pltpu.VMEM)
    anywhere = pl.BlockSpec(memory_space=pl.ANY)
    copies = (20 + 6 * heads_each) * inner
    return pl.pallas_call(
        functools.partial(fused_kernel, outer, inner),
        out_shape=(
            pltpu.VMEM(weight.shape, f32),
            pltpu.VMEM(weight.shape, f32),
            pltpu.VMEM((width, own_cols), bf16),
            pltpu.VMEM(left_stat.shape, f32),
            pltpu.VMEM(right_stat.shape, f32),
        ),
        in_specs=[pl.BlockSpec(memory_space=pltpu.SMEM)] + [vmem] + [anywhere] * 8,
        out_specs=[vmem] * 5,
        scratch_shapes=[
            pltpu.VMEM((inner, rows, width), bf16),
            pltpu.VMEM((inner, own_rows, width), bf16),
            pltpu.VMEM((inner, cols, rows), bf16),
            pltpu.VMEM((inner, cols, rows), bf16),
            pltpu.VMEM((heads_each, outer, size, chunk), bf16),
            pltpu.VMEM((heads_each, outer, size, chunk), bf16),
            pltpu.VMEM((heads_each, size, chunk), f32),
            pltpu.VMEM((outer, cols, chunk), bf16),
            pltpu.VMEM((chunk, cols), bf16),
            pltpu.VMEM((inner, own_rows, cols), bf16),
            pltpu.VMEM((inner, own_rows, cols), bf16),
            pltpu.VMEM((inner, heads_each, size, size), bf16),
            pltpu.VMEM((3, 2, 8, 128), f32),
            pltpu.VMEM((inner + outer - 1, 2, 8, 128), f32),
            pltpu.VMEM((group_rows, half), f32),
            pltpu.VMEM((group_rows, half), bf16),
            pltpu.VMEM((group_rows, half), bf16),
            pltpu.VMEM((inner - 1, own_rows, half), bf16),
            pltpu.VMEM((inner - 1, own_rows, half), bf16),
            pltpu.VMEM(values_first.shape, bf16),
            pltpu.VMEM(values_second.shape, bf16),
            pltpu.VMEM(right_root.shape, bf16),
            pltpu.VMEM(weight.shape, f32),
            pltpu.VMEM(left_stat.shape, f32),
            pltpu.VMEM(right_stat.shape, f32),
            pltpu.SemaphoreType.DMA((copies,)),
            pltpu.SemaphoreType.DMA((copies,)),
            pltpu.SemaphoreType.DMA((8,)),
        ],
        compiler_params=pltpu.CompilerParams(
            collective_id=0, has_side_effects=True, vmem_limit_bytes=56 * 1024 * 1024
        ),
        name="fused_update",
    )(
        head_lambda,
        out_gain.reshape(1, size),
        cotangent,
        values_first,
        values_second,
        left_root,
        right_root,
        weight,
        left_stat,
        right_stat,
    )


def step(*args):
    head_count, size = args[3].shape[0], args[4].shape[0]
    outer, rest = divmod(lax.axis_size("fs"), INNER)
    aligned = (
        rest == 0
        and lax.axis_size("tp") == 2
        and outer == 4
        and head_count % INNER == 0
        and size == 128
        and args[0].shape[0] % 128 == 0
        and args[5].shape[0] % 128 == 0
        and (args[0].shape[1] // outer) % 128 == 0
    )
    return tuple(fused(*args)) if aligned else shards(*args)


def solution(mesh):
    return jax.shard_map(
        step,
        mesh=mesh,
        in_specs=(
            P("fs", None),
            P("fs", "tp"),
            P("fs", "tp"),
            P("tp"),
            P(),
            P("fs", "tp"),
            P("fs", "tp"),
            P("tp", None, None),
            P("fs", None),
            P("tp", None, None),
        ),
        out_specs=(P("fs", "tp"), P("fs", "tp"), P(None, "tp"), P("fs", "tp"), P("tp", None, None)),
        check_vma=False,
    )
```

```python
import functools

import jax
import jax.numpy as jnp
from jax import lax
from jax.experimental import pallas as pl
from jax.experimental.pallas import tpu as pltpu
from jax.sharding import PartitionSpec as P

MESH = pl.DeviceIdType.MESH
INNER = 4

epsilon = 1e-06
decay_rate = 0.9
learn_rate = 0.01
output_scale = 0.2


def normalized(values_first, values_second, head_lambda, out_gain):
    token_count = values_first.shape[0]
    head_count = head_lambda.shape[0]
    head_size = out_gain.shape[0]
    first = values_first.astype(jnp.float32).reshape(token_count, head_count, head_size)
    second = values_second.astype(jnp.float32).reshape(token_count, head_count, head_size)
    difference = first - head_lambda[None, :, None] * second
    inverse = lax.rsqrt(jnp.mean(difference * difference, axis=-1, keepdims=True) + epsilon)
    scaled = difference * inverse * out_gain * output_scale
    return scaled.reshape(token_count, head_count * head_size).astype(jnp.bfloat16)


def by_head(matrix, head_count):
    return matrix.reshape(matrix.shape[0], head_count, matrix.shape[1] // head_count)


def head_products(matrix, head_count):
    heads = by_head(matrix, head_count)
    return jnp.einsum("rhi,rhj->hij", heads, heads, preferred_element_type=jnp.float32)


def shards(
    cotangent,
    values_first,
    values_second,
    head_lambda,
    out_gain,
    weight,
    left_stat,
    right_stat,
    left_root,
    right_root,
):
    head_count = head_lambda.shape[0]
    own_rows = weight.shape[0]
    own_cols = weight.shape[1]
    width = left_root.shape[1]
    total_cols = own_cols * lax.axis_size("tp")
    head_out = normalized(values_first, values_second, head_lambda, out_gain)
    contract_rows = (((0,), (0,)), ((), ()))
    contract_cols = (((1,), (1,)), ((), ()))
    gradient = lax.psum_scatter(
        lax.dot_general(cotangent, head_out, contract_rows, preferred_element_type=jnp.float32),
        "fs",
        scatter_dimension=0,
        tiled=True,
    )
    grad_half = gradient.astype(jnp.bfloat16)
    portion = lax.all_gather(grad_half, "fs", axis=0, tiled=True)
    left_acc = jnp.dot(left_root, portion, preferred_element_type=jnp.float32)
    products = lax.dot_general(
        grad_half, portion, contract_cols, preferred_element_type=jnp.float32
    )
    stat_cols = products
    right_acc = head_products(portion, head_count)
    left_acc, stat_cols, right_acc = (left_acc, stat_cols, right_acc)
    left_summed = lax.psum_scatter(
        stat_cols.astype(jnp.bfloat16), "tp", scatter_dimension=1, tiled=True
    ).astype(jnp.float32)
    new_left_stat = decay_rate * left_stat + (1.0 - decay_rate) / total_cols * left_summed
    new_right_stat = decay_rate * right_stat + (1.0 - decay_rate) / width * right_acc
    left_half = left_acc.astype(jnp.bfloat16)
    precond = jnp.einsum(
        "rhi,hij->rhj",
        by_head(left_half, head_count),
        right_root,
        preferred_element_type=jnp.float32,
    )
    precond = precond.reshape(own_rows, own_cols)
    grad_square, update_square = lax.psum(
        (jnp.sum(gradient * gradient), jnp.sum(precond * precond)), ("fs", "tp")
    )
    factor = jnp.sqrt((grad_square + epsilon) / (update_square + epsilon))
    update_step = factor * precond
    new_weight = weight - learn_rate * update_step
    new_copy = lax.all_gather(new_weight.astype(jnp.bfloat16), "fs", axis=0, tiled=True)
    return (update_step, new_weight, new_copy, new_left_stat, new_right_stat)


def dot(a, b, dims):
    return lax.dot_general(a, b, (dims, ((), ())), preferred_element_type=jnp.float32)


def fused_kernel(
    outer,
    inner,
    lam_ref,
    gain_ref,
    cot_hbm,
    first_hbm,
    second_hbm,
    root_hbm,
    right_root_hbm,
    weight_hbm,
    left_stat_hbm,
    right_stat_hbm,
    step_ref,
    new_weight_ref,
    copy_ref,
    new_left_ref,
    new_right_ref,
    cot_all,
    root_all,
    head_out,
    head_in,
    part_out,
    part_in,
    own_part,
    grad_t,
    grad_rows,
    pre_out,
    pre_in,
    prod_all,
    square_out,
    square_in,
    stat_own,
    pair_out,
    pair_in,
    stat_out,
    stat_in,
    first_ref,
    second_ref,
    rr_ref,
    w_ref,
    ls_ref,
    rs_ref,
    send_sem,
    recv_sem,
    local_sem,
):
    me = lax.axis_index("fs")
    core = lax.axis_index("tp")
    oi = me // inner
    ij = lax.rem(me, inner)
    rows, width = cot_hbm.shape
    own_rows = root_hbm.shape[0]
    size = gain_ref.shape[1]
    cols = head_in.shape[1]
    heads_each = cols // size
    chunk = width // outer
    half = width // 2
    mine = pl.ds(pl.multiple_of(core * half, half), half)

    def inner_peer(d):
        return lax.rem(ij + d, inner)

    is_mid = lax.rem((oi + 1) // 2, 2)
    near = oi + 1 - 2 * lax.rem(oi, 2)
    across = 2 - oi // 2
    far = (outer - 1) * (1 - oi // 2)
    x_peer = ij + 1 - 2 * lax.rem(ij, 2)
    y_peer = lax.rem(ij + 2, inner)

    def inner_id(d):
        return (oi * inner + inner_peer(d), core)

    def outer_id(o):
        return (o * inner + ij, core)

    def inner_at(j):
        return (oi * inner + j, core)

    sibling = (me, 1 - core)
    started = []
    started_mid = []
    used = [0]

    def fresh(count=1):
        used[0] += count
        return used[0] - count

    def describe(src, dst, device, arrival):
        return pltpu.make_async_remote_copy(
            src_ref=src,
            dst_ref=dst,
            send_sem=send_sem.at[fresh()],
            recv_sem=recv_sem.at[arrival],
            device_id=device,
            device_id_type=MESH,
        )

    arrivals = [0]

    def expect(count=1):
        arrivals[0] += count
        return arrivals[0] - count

    def send(src, dst, device, arrival=None):
        copy = describe(src, dst, device, expect() if arrival is None else arrival)
        copy.start()
        started.append(copy)
        return copy

    def arrived(ref, arrival):
        pltpu.make_async_copy(ref, ref, recv_sem.at[arrival]).wait()

    def gather_outer(block):
        base = expect(3)
        own = block(oi)
        send(own, own, outer_id(across), base + 1 + is_mid)
        direct = describe(own, own, outer_id(far), base + 2)
        relayed = describe(block(far), block(far), outer_id(near), base + 1)

        @pl.when(is_mid == 1)
        def _():
            direct.start()

        send(own, own, outer_id(near), base)
        started_mid.extend([direct, relayed])

        def wait_near():
            arrived(block(near), base)

        def wait_far():
            arrived(block(far), base + 1)

            @pl.when(is_mid == 1)
            def _():
                relayed.start()

        def wait_across():
            arrived(block(across), base + 2)

        return wait_near, wait_far, wait_across

    inner_steps = range(1, inner)
    outer_steps = range(1, outer)

    locals_ = [
        pltpu.make_async_copy(cot_hbm, cot_all.at[ij], local_sem.at[0]),
        pltpu.make_async_copy(root_hbm, root_all.at[ij], local_sem.at[1]),
        pltpu.make_async_copy(right_root_hbm, rr_ref, local_sem.at[2]),
        pltpu.make_async_copy(weight_hbm, w_ref, local_sem.at[3]),
        pltpu.make_async_copy(left_stat_hbm, ls_ref, local_sem.at[4]),
        pltpu.make_async_copy(right_stat_hbm, rs_ref, local_sem.at[5]),
        pltpu.make_async_copy(first_hbm, first_ref, local_sem.at[6]),
        pltpu.make_async_copy(second_hbm, second_ref, local_sem.at[7]),
    ]
    for index in (0, 6, 7, 1, 2, 3, 4, 5):
        locals_[index].start()

    barrier = pltpu.get_barrier_semaphore()
    peers = [inner_id(d) for d in inner_steps] + [outer_id(lax.rem(oi + d, outer)) for d in outer_steps] + [sibling]
    for peer in peers:
        pl.semaphore_signal(barrier, inc=1, device_id=peer, device_id_type=MESH)
    pl.semaphore_wait(barrier, len(peers))

    locals_[0].wait()
    own_cot = cot_all.at[ij, :, mine]
    cot_copies = [send(own_cot, own_cot, inner_id(d)) for d in inner_steps]
    locals_[6].wait()
    locals_[7].wait()

    gain = gain_ref[...] * output_scale
    for h in range(inner * heads_each):
        span = slice(h * size, (h + 1) * size)
        first = first_ref[:, span].astype(jnp.float32)
        second = second_ref[:, span].astype(jnp.float32)
        difference = first - lam_ref[h] * second
        inverse = lax.rsqrt(jnp.mean(difference * difference, axis=-1, keepdims=True) + epsilon)
        scaled = difference * inverse * gain
        k = h % heads_each
        head_out[h // heads_each, k * size : (k + 1) * size, :] = scaled.T.astype(jnp.bfloat16)
    head_copies = [
        send(head_out.at[inner_peer(d)], head_in.at[ij], inner_id(d)) for d in inner_steps
    ]
    head_in[ij] = head_out[ij]

    def forward(copies, buffer):
        result = []
        for d, copy in zip(inner_steps, copies):
            copy.wait_recv()
            place = buffer.at[lax.rem(ij + inner - d, inner), :, mine]
            result.append(send(place, place, sibling))
        return result

    cot_pair = forward(cot_copies, cot_all)
    for copy in head_copies:
        copy.wait_recv()
    locals_[1].wait()
    own_root = root_all.at[ij, :, mine]
    root_copies = [send(own_root, own_root, inner_id(d)) for d in inner_steps]
    for copy in cot_pair:
        copy.wait_recv()

    def head(k):
        return slice(k * size, (k + 1) * size)

    heads = range(heads_each)
    lhs = [jnp.concatenate([head_in[j, head(k), :] for j in range(inner)], axis=1) for k in heads]

    def part(owner, k):
        span = pl.ds(pl.multiple_of(owner * chunk, chunk), chunk)
        rhs = cot_all[:, :, span].reshape(inner * rows, chunk)
        return dot(lhs[k], rhs, ((1,), (0,)))

    slot = 2 - is_mid
    bases, to_relay, combined = [], [], []
    for k in heads:
        base = expect(4)
        bases.append(base)
        part_out[k, 0] = part(far, k).astype(jnp.bfloat16)
        copy = describe(part_out.at[k, 0], part_in.at[k, 3], outer_id(near), base + 3)
        to_relay.append(copy)

        @pl.when(is_mid == 0)
        def _():
            copy.start()

        part_out[k, 1] = part(across, k).astype(jnp.bfloat16)
        send(part_out.at[k, 1], part_in.at[k, slot], outer_id(across), base + slot)
        part_out[k, 2] = part(near, k).astype(jnp.bfloat16)
        send(part_out.at[k, 2], part_in.at[k, 0], outer_id(near), base)
    for k in heads:
        copy = describe(part_out.at[k, 3], part_in.at[k, 1], outer_id(far), bases[k] + 1)
        combined.append(copy)

        @pl.when(is_mid == 1)
        def _():
            arrived(part_in.at[k, 3], bases[k] + 3)
            total_far = part_out[k, 0].astype(jnp.float32) + part_in[k, 3].astype(jnp.float32)
            part_out[k, 3] = total_far.astype(jnp.bfloat16)
            copy.start()

    for k in heads:
        own_part[k] = part(oi, k)
    grad_square = jnp.zeros((), jnp.float32)
    grad_waits = []
    for k in heads:
        base = bases[k]
        arrived(part_in.at[k, 0], base)
        own_part[k] += part_in[k, 0].astype(jnp.float32)

        @pl.when(is_mid == 1)
        def _():
            arrived(part_in.at[k, 2], base + 2)
            own_part[k] += part_in[k, 2].astype(jnp.float32)

        arrived(part_in.at[k, 1], base + 1)
        gradient = own_part[k] + part_in[k, 1].astype(jnp.float32)
        own_part[k] = gradient
        grad_t[oi, head(k), :] = gradient.astype(jnp.bfloat16)
        grad_waits.append(gather_outer(lambda o, k=k: grad_t.at[o, head(k), :]))
    for k in heads:
        gradient = own_part[k]
        grad_square = grad_square + jnp.sum(gradient * gradient)
        grad_rows[:, head(k)] = gradient.T.astype(jnp.bfloat16)
    square_out[0, 0] = jnp.full((8, 128), grad_square, jnp.float32)

    root_pair = forward(root_copies, root_all)
    grad_waits[0][1]()
    for copy in root_pair:
        copy.wait_recv()
    locals_[2].wait()

    total = jnp.zeros((1, 1), jnp.float32)
    for k in heads:
        wait_near, wait_far, wait_across = grad_waits[k]
        wait_near()
        wait_across()
        if k + 1 < heads_each:
            grad_waits[k + 1][1]()
        acc = jnp.zeros((inner * own_rows, size), jnp.float32)
        for o in range(outer):
            block = root_all[:, :, o * chunk : (o + 1) * chunk].reshape(inner * own_rows, chunk)
            acc = acc + dot(block, grad_t[o, head(k), :], ((1,), (1,)))
        precond = dot(acc.astype(jnp.bfloat16), rr_ref[ij * heads_each + k], ((1,), (0,)))
        total = total + jnp.sum(precond * precond)
        for j in range(inner):
            pre_out[j, :, head(k)] = precond[j * own_rows : (j + 1) * own_rows].astype(jnp.bfloat16)
    pre_copies = [send(pre_out.at[inner_peer(d)], pre_in.at[ij], inner_id(d)) for d in inner_steps]
    pre_in[ij] = pre_out[ij]
    square_out[0, 1] = jnp.broadcast_to(total, (8, 128))
    square_copy = send(square_out.at[0], square_in.at[0], sibling)

    def stat_part(core_half, k):
        return dot(grad_rows[...], grad_t[core_half * (outer // 2) + k], ((1,), (0,)))

    for k in range(outer // 2):
        pair_out[:, k * chunk : (k + 1) * chunk] = stat_part(1 - core, k).astype(jnp.bfloat16)
    pair_copy = send(pair_out, pair_in, sibling)

    square_copy.wait_recv()
    square_out[1] = square_out[0] + square_in[0]
    square_copies = [
        send(square_out.at[1], square_in.at[d], inner_id(d)) for d in inner_steps
    ]
    for k in range(heads_each):
        product = jnp.zeros((size, size), jnp.float32)
        for o in range(outer):
            piece = grad_t[o, k * size : (k + 1) * size, :]
            product = product + dot(piece, piece, ((1,), (1,)))
        prod_all[ij, k] = product.astype(jnp.bfloat16)
    prod_copies = [send(prod_all.at[ij], prod_all.at[ij], inner_id(d)) for d in inner_steps]

    squares = square_out[1]
    for d, copy in zip(inner_steps, square_copies):
        copy.wait_recv()
        squares = squares + square_in[d]
    square_out[2] = squares
    square_copies = [
        send(
            square_out.at[2],
            square_in.at[inner + d - 1],
            outer_id(lax.rem(oi + d, outer)),
        )
        for d in outer_steps
    ]
    for k in range(outer // 2):
        stat_own[:, k * chunk : (k + 1) * chunk] = stat_part(core, k)

    pair_copy.wait_recv()
    stat_copies = []
    for d in tuple(inner_steps) + (0,):
        span = pl.ds(pl.multiple_of(inner_peer(d) * own_rows, own_rows), own_rows)
        summed = stat_own[span, :] + pair_in[span, :].astype(jnp.float32)
        if d:
            stat_out[d - 1] = summed.astype(jnp.bfloat16)
            stat_copies.append(send(stat_out.at[d - 1], stat_in.at[d - 1], inner_id(d)))
        else:
            stat_own[span, :] = summed

    for copy in pre_copies:
        copy.wait_recv()
    locals_[3].wait()
    for d, copy in zip(outer_steps, square_copies):
        copy.wait_recv()
        squares = squares + square_in[inner + d - 1]
    factor = jnp.sqrt((squares[0] + epsilon) / (squares[1] + epsilon))[0:1, 0:1]

    def rows_of(o, j):
        return pl.ds(pl.multiple_of((o * inner + j) * own_rows, own_rows), own_rows)

    place = rows_of(oi, ij)
    for j in range(inner):
        span = slice(j * cols, (j + 1) * cols)
        step = factor * pre_in[j].astype(jnp.float32)
        updated = w_ref[:, span] - learn_rate * step
        step_ref[:, span] = step
        new_weight_ref[:, span] = updated
        copy_ref[place, span] = updated.astype(jnp.bfloat16)
    main = own_rows * 5 // 8
    rest = own_rows - main

    def piece(o, j, start, count):
        place = (o * inner + j) * own_rows + start
        return copy_ref.at[pl.ds(pl.multiple_of(place, own_rows // 8), count), :]

    last = []

    def spread(o, start, count):
        block = piece(o, ij, start, count)
        to_x = send(block, block, inner_at(x_peer))
        to_y = send(block, block, inner_at(y_peer))
        return o, start, count, to_x, to_y

    def pass_on(flight, flip=False):
        o, start, count, from_x, from_y = flight
        unit = own_rows // 8
        part_rows = (count // unit + 1) // 2 * unit
        if flip:
            part_rows = count - part_rows
        from_x.wait_recv()
        block = piece(o, x_peer, start, part_rows)
        one = send(block, block, inner_at(y_peer))
        from_y.wait_recv()
        block = piece(o, y_peer, start + part_rows, count - part_rows)
        return one, send(block, block, inner_at(x_peer))

    def gather_rest(j):
        return gather_outer(lambda o: piece(o, j, main, rest))

    rest_flight = spread(oi, main, rest)
    near_in, far_in, across_in = gather_outer(lambda o: piece(o, ij, 0, main))
    flight = spread(oi, 0, main)
    rest_waits = [gather_rest(ij)]
    rest_last = pass_on(rest_flight)
    rest_waits += [gather_rest(x_peer), gather_rest(y_peer)]
    near_in()
    near_flight = spread(near, 0, main)
    far_in()
    last += pass_on(flight, True)
    for copy in rest_last:
        copy.wait_recv()
    rest_waits.append(gather_rest(inner - 1 - ij))
    across_in()
    across_flight = spread(across, 0, main)
    rest_waits[0][1]()
    far_flight = spread(far, 0, main)
    last += pass_on(near_flight)
    rest_waits[1][1]()
    rest_waits[2][1]()
    last += pass_on(across_flight, True)
    rest_waits[3][1]()
    last += pass_on(far_flight)

    for copy in prod_copies:
        copy.wait_recv()
    locals_[5].wait()
    for j in range(inner):
        for k in range(heads_each):
            h = j * heads_each + k
            new_right_ref[h] = decay_rate * rs_ref[h] + (1.0 - decay_rate) / width * prod_all[
                j, k
            ].astype(jnp.float32)
    locals_[4].wait()
    for copy in stat_copies:
        copy.wait_recv()
    stat_sum = stat_own[pl.ds(pl.multiple_of(ij * own_rows, own_rows), own_rows), :]
    for d in inner_steps:
        stat_sum = stat_sum + stat_in[d - 1].astype(jnp.float32)
    scale = (1.0 - decay_rate) / (2 * inner * cols)
    new_left_ref[...] = decay_rate * ls_ref[...] + scale * stat_sum
    for copy in last:
        copy.wait_recv()
    for near_in, _, across_in in rest_waits:
        near_in()
        across_in()
    for copy in started:
        copy.wait_send()

    @pl.when(is_mid == 1)
    def _():
        for copy in combined + started_mid:
            copy.wait_send()

    @pl.when(is_mid == 0)
    def _():
        for copy in to_relay:
            copy.wait_send()


def fused(
    cotangent,
    values_first,
    values_second,
    head_lambda,
    out_gain,
    weight,
    left_stat,
    right_stat,
    left_root,
    right_root,
):
    inner = INNER
    outer = lax.axis_size("fs") // inner
    rows, width = cotangent.shape
    own_rows, own_cols = weight.shape
    size = out_gain.shape[0]
    cols = own_cols // inner
    heads_each = cols // size
    chunk = width // outer
    half = width // 2
    group_rows = inner * own_rows
    bf16, f32 = jnp.bfloat16, jnp.float32
    vmem = pl.BlockSpec(memory_space=pltpu.VMEM)
    anywhere = pl.BlockSpec(memory_space=pl.ANY)
    copies = (20 + 6 * heads_each) * inner
    return pl.pallas_call(
        functools.partial(fused_kernel, outer, inner),
        out_shape=(
            pltpu.VMEM(weight.shape, f32),
            pltpu.VMEM(weight.shape, f32),
            pltpu.VMEM((width, own_cols), bf16),
            pltpu.VMEM(left_stat.shape, f32),
            pltpu.VMEM(right_stat.shape, f32),
        ),
        in_specs=[pl.BlockSpec(memory_space=pltpu.SMEM)] + [vmem] + [anywhere] * 8,
        out_specs=[vmem] * 5,
        scratch_shapes=[
            pltpu.VMEM((inner, rows, width), bf16),
            pltpu.VMEM((inner, own_rows, width), bf16),
            pltpu.VMEM((inner, cols, rows), bf16),
            pltpu.VMEM((inner, cols, rows), bf16),
            pltpu.VMEM((heads_each, outer, size, chunk), bf16),
            pltpu.VMEM((heads_each, outer, size, chunk), bf16),
            pltpu.VMEM((heads_each, size, chunk), f32),
            pltpu.VMEM((outer, cols, chunk), bf16),
            pltpu.VMEM((chunk, cols), bf16),
            pltpu.VMEM((inner, own_rows, cols), bf16),
            pltpu.VMEM((inner, own_rows, cols), bf16),
            pltpu.VMEM((inner, heads_each, size, size), bf16),
            pltpu.VMEM((3, 2, 8, 128), f32),
            pltpu.VMEM((inner + outer - 1, 2, 8, 128), f32),
            pltpu.VMEM((group_rows, half), f32),
            pltpu.VMEM((group_rows, half), bf16),
            pltpu.VMEM((group_rows, half), bf16),
            pltpu.VMEM((inner - 1, own_rows, half), bf16),
            pltpu.VMEM((inner - 1, own_rows, half), bf16),
            pltpu.VMEM(values_first.shape, bf16),
            pltpu.VMEM(values_second.shape, bf16),
            pltpu.VMEM(right_root.shape, bf16),
            pltpu.VMEM(weight.shape, f32),
            pltpu.VMEM(left_stat.shape, f32),
            pltpu.VMEM(right_stat.shape, f32),
            pltpu.SemaphoreType.DMA((copies,)),
            pltpu.SemaphoreType.DMA((copies,)),
            pltpu.SemaphoreType.DMA((8,)),
        ],
        compiler_params=pltpu.CompilerParams(
            collective_id=0, has_side_effects=True, vmem_limit_bytes=56 * 1024 * 1024
        ),
        name="fused_update",
    )(
        head_lambda,
        out_gain.reshape(1, size),
        cotangent,
        values_first,
        values_second,
        left_root,
        right_root,
        weight,
        left_stat,
        right_stat,
    )


def step(*args):
    head_count, size = args[3].shape[0], args[4].shape[0]
    outer, rest = divmod(lax.axis_size("fs"), INNER)
    aligned = (
        rest == 0
        and lax.axis_size("tp") == 2
        and outer == 4
        and head_count % INNER == 0
        and size == 128
        and args[0].shape[0] % 128 == 0
        and args[5].shape[0] % 128 == 0
        and (args[0].shape[1] // outer) % 128 == 0
    )
    return tuple(fused(*args)) if aligned else shards(*args)


def solution(mesh):
    return jax.shard_map(
        step,
        mesh=mesh,
        in_specs=(
            P("fs", None),
            P("fs", "tp"),
            P("fs", "tp"),
            P("tp"),
            P(),
            P("fs", "tp"),
            P("fs", "tp"),
            P("tp", None, None),
            P("fs", None),
            P("tp", None, None),
        ),
        out_specs=(P("fs", "tp"), P("fs", "tp"), P(None, "tp"), P("fs", "tp"), P("tp", None, None)),
        check_vma=False,
    )
```
